32 devices in a mesh: sp: 8 (over z, x), tp: 4 (over y, core).
Axes of the slice: x: 2, y: 2, z: 4, core: 2. Of those that a mesh axis runs over, the one named last changes fastest.
Arguments:
- residual: bfloat16 [1024, 2048], P('sp', 'tp'), may hold values from -80 to 80
- query_wide: bfloat16 [1024, 1024], P('sp', 'tp'), may hold values from -6 to 6
- key_wide: bfloat16 [1024, 1024], P('sp', 'tp'), may hold values from -6 to 6
- query_narrow: bfloat16 [1024, 512], P('sp', 'tp'), may hold values from -6 to 6
- key_narrow: bfloat16 [1024, 512], P('sp', 'tp'), may hold values from -6 to 6
- values: bfloat16 [1024, 2048], P('sp', 'tp'), may hold values from -6 to 6
- gate_logits: float32 [4, 8, 1024], P(None, 'tp', 'sp'), may hold values from -6 to 106
- head_gain: float32 [2048], P('tp'), may hold values from 0.1 to 1.9
- norm_gain: float32 [2048], replicated, may hold values from 0.1 to 1.9
- route_experts: int32 [1024, 2], P('sp'), may hold values from 0 to 7, all different within a row; in each aligned block of 128 rows (0 to 127, 128 to 255, ...) at most 64 rows name the same one
- route_weights: float32 [1024, 2], P('sp'), may hold values from 0.2 to 1
- expert_gate: bfloat16 [8, 2048, 3584], P('sp', None, 'tp'), may hold values from -0.125 to 0.125
- expert_up: bfloat16 [8, 2048, 3584], P('sp', None, 'tp'), may hold values from -0.125 to 0.125
- expert_down: bfloat16 [8, 3584, 2048], P('sp', 'tp'), may hold values from -0.09375 to 0.09375
Outputs:
- layer_out: bfloat16 [1024, 2048], P('sp', 'tp')
The draws below stay inside these ranges and needn't reach their ends.
Inputs may be any that keep to these rules, and one draw needn't show every extreme that they name: `route_experts`: each row names 2 different experts; within the rows of one device (aligned blocks of 128 rows) no expert is named more than 64 times, a bound that some block reaches.
All inputs are finite; a program needn't handle non-finite values.
Results may differ from the reference program's by a relative error of at most 0.0055.
Values may be sent and summed in bfloat16 or wider, within the bound.
No kernel may reach another device: no remote copies, remote signals or barrier semaphores. Data moves between devices by JAX's collectives and lax.ppermute only.
A program may use at most 128 MiB of HBM per device.

```python
import math
import jax
import jax.numpy as jnp
import numpy as np
from jax import lax

HEADS = 4
DKW = 256
DKN = 128
DV = 256
FF = 3584
TOP = 2
BLOCK = 64
TOK_DEV = 128
D = 2048
TOKENS = 1024
EXPERTS = 8
CAP = 64
N_SP = 8
N_TP = 4


def draw_residual(key, part):
    first, second = jax.random.split(key, 2)
    column_log = jax.random.uniform(second, (16,), jnp.float32, -1.2, 1.2)
    column_scale = jnp.exp(jnp.repeat(column_log, D // 16))
    noise = jnp.clip(jax.random.normal(first, (TOKENS, D), jnp.float32), -6.0, 6.0)
    return (noise * column_scale[None, :]).astype(jnp.bfloat16)


def draw_gate_logits(key, part):
    subkeys = jax.random.split(key, 3)
    head_total = 2 * HEADS
    noise = jnp.clip(jax.random.normal(subkeys[0], (4, head_total, TOKENS), jnp.float32), -4.0, 4.0)
    span_count = TOKENS // TOK_DEV
    block_shift = jax.random.uniform(subkeys[1], (4, head_total, span_count), jnp.float32, -0.9, 0.9)
    block_shift = jnp.repeat(block_shift, TOK_DEV, axis=2)
    ranking = jnp.stack([jax.random.permutation(jax.random.fold_in(subkeys[2], side), head_total) for side in range(2)])
    quick = (ranking < head_total // 2).astype(jnp.float32)
    keep_base = 11.5 - 8.0 * quick
    forget = keep_base[:, :, None] + 0.7 * noise[1::2] + block_shift[1::2]
    incoming = 1.2 * noise[0::2] + block_shift[0::2]
    return jnp.stack([incoming[0], forget[0], incoming[1], forget[1]])


def level_of(rng, dims, pieces, least, top_value):
    gain = 1.0
    for axis_at, shards_of in pieces:
        draws = jax.random.uniform(jax.random.fold_in(jax.random.fold_in(rng, 6), axis_at), (shards_of,), jnp.float32, least / len(pieces), top_value / len(pieces))
        gain = gain * jnp.repeat(jnp.exp(draws), dims[axis_at] // shards_of).reshape((-1,) + (1,) * (len(dims) - 1 - axis_at))
    return gain


def shared_out(rng, own, number, rows, amount, top, reach, skew):
    sequence = jax.random.permutation(rng, amount)
    heavy_load, usual = shares(amount, rows * top, reach, skew, True), shares(amount, rows * top, reach, skew, False)
    places = jnp.arange(amount)

    def named(tallies, offset_by):
        used = int((tallies > 0).sum())
        fixed = max(1, used // 4)
        moved = fixed + (places - fixed + offset_by * (used - fixed)) % max(1, amount - fixed)
        return jnp.zeros((amount,), jnp.int32).at[sequence[jnp.where(places < fixed, places, moved)]].set(jnp.asarray(tallies, jnp.int32))

    tallies = jnp.where(number % 4 == 0, named(heavy_load, number // 4), named(usual, number - number // 4 - 1))
    mixed = jax.random.permutation(jax.random.fold_in(own, 3), amount)
    source_of, taker = mixed[0:amount // 2 * 2:2], mixed[1:amount // 2 * 2:2]
    slack = jnp.minimum(tallies[source_of] - 1, reach - tallies[taker]) // 2
    slack = jnp.where((source_of == sequence[0]) | (taker == sequence[0]) | (tallies[taker] == 0), 0, jnp.maximum(slack, 0))
    moved = jax.random.randint(jax.random.fold_in(own, 4), (amount // 2,), 0, 1 << 20) % (slack + 1)
    tallies = tallies.at[source_of].add(-moved).at[taker].add(moved)
    labels = jnp.searchsorted(jnp.cumsum(tallies), jnp.arange(rows * top), side="right").astype(jnp.int32)
    table = labels.reshape(top, rows).T
    table = table[jax.random.permutation(jax.random.fold_in(own, 1), rows)]
    offset_by = jax.random.randint(jax.random.fold_in(own, 2), (rows, 1), 0, top)
    return jnp.take_along_axis(table, (jnp.arange(top)[None, :] + offset_by) % top, axis=1)


def shares(number_of, total, bound, slope, full):
    weights = [(1 << 20) // math.isqrt(rank ** slope) + 1 for rank in range(1, number_of + 1)]
    largest = bound if full else min(bound, max(-(-total // number_of), total * weights[0] // sum(weights)))
    least = 1 if total - largest >= number_of - 1 else 0
    holding, spare = [largest] + [least] * (number_of - 1), total - largest - least * (number_of - 1)
    while spare > 0:
        candidates = [i for i in range(1, number_of) if holding[i] < largest] or [i for i in range(1, number_of) if holding[i] < bound]
        pool, budget = sum([weights[i] for i in candidates]), spare
        for i in candidates:
            extra = min(bound - holding[i], max(1, budget * weights[i] // pool), spare)
            holding[i] = holding[i] + extra
            spare = spare - extra
    return np.array(holding)


def gaussian(key, extent, width, limit, cuts=(), held_as=jnp.bfloat16):
    entries = jax.random.normal(key, extent, jnp.float32) * width
    if len(cuts) > 0:
        entries = level_of(key, extent, cuts, -0.22, 0.18) * entries
    return jnp.clip(entries, min=-limit, max=limit).astype(held_as)


def setup_inputs(seed: int = 0) -> dict:
    arg_keys = jax.random.split(jax.random.key(seed), 15)
    residual = draw_residual(jax.random.fold_in(arg_keys[14], 71), 0)
    query_wide = gaussian(arg_keys[1], (TOKENS, HEADS * DKW), 1.0, 6.0, ((0, 8), (1, 4)))
    key_wide = gaussian(arg_keys[2], (TOKENS, HEADS * DKW), 1.0, 6.0, ((0, 8), (1, 4)))
    query_narrow = gaussian(arg_keys[3], (TOKENS, HEADS * DKN), 1.0, 6.0, ((0, 8), (1, 4)))
    key_narrow = gaussian(arg_keys[4], (TOKENS, HEADS * DKN), 1.0, 6.0, ((0, 8), (1, 4)))
    values = gaussian(arg_keys[5], (TOKENS, D), 1.0, 6.0, ((0, 8), (1, 4)))
    gate_logits = draw_gate_logits(jax.random.fold_in(arg_keys[14], 71), 0)
    head_gain = jnp.clip(1.0 + 0.18 * jax.random.normal(arg_keys[7], (D,), jnp.float32), 0.1, 1.9)
    norm_gain = jnp.clip(1.0 + 0.18 * jax.random.normal(arg_keys[8], (D,), jnp.float32), 0.1, 1.9)
    route_experts_keys = jax.random.split(jax.random.fold_in(arg_keys[9], 1), TOKENS // TOK_DEV)
    route_experts_turns = jax.random.permutation(jax.random.fold_in(arg_keys[9], 3), TOKENS // TOK_DEV)
    route_experts = jax.vmap(lambda own, number: shared_out(jax.random.fold_in(arg_keys[9], 2), own, number, TOK_DEV, EXPERTS, TOP, CAP, 1))(route_experts_keys, route_experts_turns).reshape((TOKENS, TOP))
    route_weights = jnp.clip(0.2 + 0.8 * jax.random.uniform(arg_keys[10], (TOKENS, TOP), jnp.float32) ** level_of(arg_keys[10], (TOKENS, TOP), ((0, 8),), -0.2, 0.2), 0.2, 1.0)
    expert_gate = gaussian(arg_keys[11], (EXPERTS, D, FF), D ** -0.5, 0.125, ((0, 8), (2, 4)))
    expert_up = gaussian(arg_keys[12], (EXPERTS, D, FF), D ** -0.5, 0.125, ((0, 8), (2, 4)))
    expert_down = gaussian(arg_keys[13], (EXPERTS, FF, D), FF ** -0.5, 0.09375, ((0, 8), (1, 4)))
    return {"residual": residual, "query_wide": query_wide, "key_wide": key_wide, "query_narrow": query_narrow, "key_narrow": key_narrow, "values": values, "gate_logits": gate_logits, "head_gain": head_gain, "norm_gain": norm_gain, "route_experts": route_experts, "route_weights": route_weights, "expert_gate": expert_gate, "expert_up": expert_up, "expert_down": expert_down}


precise = lax.Precision.HIGHEST
norm_eps = 1e-06

def blockwise(query_heads, key_heads, value_heads, log_in, log_keep):
    head_count, length, key_width = query_heads.shape
    value_width = value_heads.shape[-1]
    block_count = length // BLOCK

    def to_blocks(array):
        return jnp.moveaxis(array.reshape((head_count, block_count, BLOCK) + array.shape[2:]), 1, 0)
    inputs = (to_blocks(query_heads), to_blocks(key_heads), to_blocks(value_heads), to_blocks(log_in), to_blocks(log_keep))
    lower_mask = jnp.tril(jnp.ones((BLOCK, BLOCK), dtype=bool))

    def advance(carried, block_in):
        memory, normer, stabilizer = carried
        query_b, key_b, value_b, in_b, keep_b = block_in
        running = jnp.cumsum(keep_b, axis=-1)
        log_weights = jnp.where(lower_mask[None], running[:, :, None] - running[:, None, :] + in_b[:, None, :], -jnp.inf)
        carry_log = running + stabilizer[:, None]
        highest = jnp.maximum(carry_log, lax.optimization_barrier(jnp.max(log_weights, axis=-1)))
        carry_w = jnp.exp(carry_log - highest)
        scores = jnp.einsum('hld,hsd->hls', query_b, key_b, precision=precise)
        intra_w = jnp.exp(log_weights - highest[:, :, None]) * scores
        numerator = carry_w[..., None] * jnp.einsum('hld,hde->hle', query_b, memory, precision=precise) + jnp.einsum('hls,hse->hle', intra_w, value_b, precision=precise)
        divisor = carry_w * jnp.einsum('hld,hd->hl', query_b, normer, precision=precise) + lax.optimization_barrier(jnp.sum(intra_w, axis=-1))
        output = numerator / jnp.maximum(jnp.abs(divisor), jnp.exp(-highest))[..., None]
        total_log = running[:, -1]
        later_log = total_log[:, None] - running + in_b
        new_stab = jnp.maximum(total_log + stabilizer, lax.optimization_barrier(jnp.max(later_log, axis=-1)))
        decay_old = jnp.exp(total_log + stabilizer - new_stab)
        weighted = key_b * jnp.exp(later_log - new_stab[:, None])[..., None]
        memory = decay_old[:, None, None] * memory + jnp.einsum('hsd,hse->hde', weighted, value_b, precision=precise)
        normer = decay_old[:, None] * normer + lax.optimization_barrier(jnp.sum(weighted, axis=1))
        return ((memory, normer, new_stab), output)
    start = (jnp.zeros((head_count, key_width, value_width), jnp.float32), jnp.zeros((head_count, key_width), jnp.float32), jnp.full((head_count,), -jnp.inf, jnp.float32))
    _, results = lax.scan(advance, start, inputs)
    return jnp.moveaxis(results, 0, 1).reshape(head_count, length, value_width)

def reverse_seq(array):
    return jnp.flip(array, axis=1)

def reference(residual, query_wide, key_wide, query_narrow, key_narrow, values, gate_logits, head_gain, norm_gain, route_experts, route_weights, expert_gate, expert_up, expert_down):
    value_all = values.astype(jnp.float32).reshape(TOKENS, HEADS, 2, DV)
    results = []
    for group_index, (query_in, key_in, key_width) in enumerate(((query_wide, key_wide, DKW), (query_narrow, key_narrow, DKN))):
        query_heads = query_in.astype(jnp.float32).reshape(TOKENS, HEADS, key_width).transpose(1, 0, 2)
        key_heads = key_in.astype(jnp.float32).reshape(TOKENS, HEADS, key_width).transpose(1, 0, 2) * key_width ** (-0.5)
        value_heads = value_all[:, :, group_index].transpose(1, 0, 2)
        gates_here = gate_logits[:, group_index::2]
        forward = blockwise(query_heads, key_heads, value_heads, gates_here[0], jax.nn.log_sigmoid(gates_here[1]))
        backward = reverse_seq(blockwise(reverse_seq(query_heads), reverse_seq(key_heads), reverse_seq(value_heads), reverse_seq(gates_here[2]), reverse_seq(jax.nn.log_sigmoid(gates_here[3]))))
        results.append(forward + backward)
    stacked = jnp.stack(results, axis=1)
    stacked = stacked * lax.rsqrt(lax.optimization_barrier(jnp.mean(stacked * stacked, axis=-1, keepdims=True)) + norm_eps)
    stacked = stacked * head_gain.reshape(HEADS, 2, 1, DV)
    heads_out = stacked.transpose(2, 0, 1, 3).reshape(TOKENS, D)
    merged = (residual.astype(jnp.float32) + heads_out).astype(jnp.bfloat16)
    merged_f = merged.astype(jnp.float32)
    normed = (merged_f * lax.rsqrt(lax.optimization_barrier(jnp.mean(merged_f * merged_f, axis=-1, keepdims=True)) + norm_eps) * norm_gain).astype(jnp.bfloat16)
    capacity = N_SP * CAP
    quarter = FF // N_TP

    def expert_step(expert, accumulated):
        chosen = route_experts == expert
        weight_row = lax.optimization_barrier(jnp.sum(jnp.where(chosen, route_weights, 0.0), axis=1))
        taken = jnp.any(chosen, axis=1)
        row_index = jnp.nonzero(taken, size=capacity, fill_value=0)[0].astype(jnp.int32)
        occupied = jnp.arange(capacity) < jnp.sum(taken.astype(jnp.int32))
        features = normed[row_index]
        gate_proj = jnp.dot(features, expert_gate[expert], preferred_element_type=jnp.float32)
        up_proj = jnp.dot(features, expert_up[expert], preferred_element_type=jnp.float32)
        hidden = (jax.nn.silu(gate_proj) * up_proj).astype(jnp.bfloat16)
        summed = jnp.zeros((capacity, D), jnp.float32)
        for block_index in range(N_TP):
            partial_sum = jnp.dot(hidden[:, block_index * quarter:(block_index + 1) * quarter], expert_down[expert, block_index * quarter:(block_index + 1) * quarter], preferred_element_type=jnp.float32)
            summed = summed + lax.optimization_barrier(partial_sum.astype(jnp.bfloat16)).astype(jnp.float32)
        result = lax.optimization_barrier(summed.astype(jnp.bfloat16)).astype(jnp.float32)
        mix_weight = jnp.where(occupied, weight_row[row_index], 0.0)
        return accumulated.at[row_index].add(result * mix_weight[:, None])
    added = lax.fori_loop(0, EXPERTS, expert_step, jnp.zeros((TOKENS, D), jnp.float32))
    return (merged_f + added).astype(jnp.bfloat16)
```

```python
import functools

import jax
import jax.numpy as jnp
from jax import lax
from jax.experimental import pallas as pl
from jax.experimental.pallas import tpu as pltpu
from jax.sharding import PartitionSpec as P

norm_eps = 1e-06
low = -1e30
tiny = 1.2e-38
f32 = jnp.float32
bf16 = jnp.bfloat16


def whole_specs(count):
    return [pl.BlockSpec(memory_space=pltpu.VMEM)] * count


def call(kernel, outs, ins, scratch=(), flops=0, nbytes=0):
    return pl.pallas_call(
        kernel,
        out_shape=outs,
        in_specs=whole_specs(len(ins)),
        out_specs=jax.tree.map(lambda _: pl.BlockSpec(memory_space=pltpu.VMEM), outs),
        scratch_shapes=list(scratch),
        cost_estimate=pl.CostEstimate(flops=flops, bytes_accessed=nbytes, transcendentals=0),
        compiler_params=pltpu.CompilerParams(vmem_limit_bytes=40 * 1024 * 1024),
    )(*ins)


def split3(value):
    first = value.astype(bf16)
    rest = value - first.astype(f32)
    second = rest.astype(bf16)
    third = (rest - second.astype(f32)).astype(bf16)
    return first, second, third


def dot3(value, ones):
    return sum(jnp.dot(part, ones, preferred_element_type=f32) for part in split3(value))


def iota(shape, dim):
    return lax.broadcasted_iota(jnp.int32, shape, dim)


def pack_kernel(key_wide, key_narrow, values, gates, out):
    rows = key_wide.shape[0]
    first = key_wide.shape[1]
    second = first + key_narrow.shape[1]
    out[:rows, :first] = key_wide[...]
    out[:rows, first:second] = key_narrow[...]
    out[:rows, second:] = values[...]
    planes, heads, _ = gates.shape
    out[rows:, :] = jnp.zeros((planes * heads, out.shape[1]), bf16)
    for plane in range(planes):
        part = gates[plane]
        if plane % 2 == 1:
            part = jnp.minimum(part, 0.0) - jnp.log1p(jnp.exp(-jnp.abs(part)))
        start = rows + plane * heads
        for index, piece in enumerate(split3(part)):
            out[start : start + heads, index * rows : (index + 1) * rows] = piece


def route_table(routes, experts):
    tops, rows = routes.shape
    expert_ids = iota((experts, rows), 0)
    taken = routes[0:1, :] == expert_ids
    for pick in range(1, tops):
        taken = taken | (routes[pick : pick + 1, :] == expert_ids)
    earlier = (iota((rows, rows), 0) < iota((rows, rows), 1)).astype(bf16)
    flags = taken.astype(f32)
    rank = jnp.dot(flags.astype(bf16), earlier, preferred_element_type=f32)
    return jnp.where(flags > 0.5, rank, -1.0)


def select_rows(table_ref, expert, capacity):
    slot = table_ref[pl.ds(expert, 1), :]
    rows = slot.shape[1]
    return (iota((capacity, rows), 0).astype(f32) == slot).astype(f32).astype(bf16)


def cell_kernel(heads, wide, narrow, width, chunks, capacity, *refs):
    query_wide, query_narrow, residual, gain, routes = refs[:5]
    blocks = refs[5 : 5 + chunks]
    merged = refs[5 + chunks]
    sent = refs[6 + chunks : 6 + 2 * chunks]
    gate_all, decay_all, weighted, table = refs[6 + 2 * chunks :]
    rows = query_wide.shape[0]
    here = lax.axis_index("sp")
    line = here // 2
    side = here % 2
    lines = chunks // 2
    sources = []
    for turn in range(lines):
        for flip in range(2):
            sources.append(lax.rem(line + lines - turn, lines) * 2 + (side + flip) % 2)
    gate_rows = 8 * heads

    def gates_of(block):
        total = None
        for part in range(3):
            piece = block[rows : rows + gate_rows, part * rows : (part + 1) * rows].astype(f32)
            total = piece if total is None else total + piece
        return total

    own = gates_of(blocks[0])
    for source, block in zip(sources, blocks):
        parts = own if block is blocks[0] else gates_of(block)
        for row in range(gate_rows):
            gate_all[row, pl.ds(source, 1), :] = parts[row : row + 1, :]

    at_row, at_col = iota((rows, rows), 0), iota((rows, rows), 1)
    later = (at_row > at_col).astype(f32).astype(bf16)
    earlier = (at_row < at_col).astype(f32).astype(bf16)
    upto = (at_row <= at_col).astype(f32).astype(bf16)
    chunk_at = iota((chunks, rows), 0)
    is_before, is_after = chunk_at < here, chunk_at > here
    own_upto = dot3(own, upto)
    own_before = dot3(own, earlier)
    gain_all = gain[...]

    for head in range(2 * heads):
        pair = head // 2
        in_row = [plane * 2 * heads + head for plane in range(4)]
        in_fwd, keep_fwd, in_bwd, keep_bwd = (gate_all[row] for row in in_row)
        total_fwd = jnp.where(is_before, jnp.sum(keep_fwd, axis=1, keepdims=True), 0.0)
        total_bwd = jnp.where(is_after, jnp.sum(keep_bwd, axis=1, keepdims=True), 0.0)
        exponent_fwd = dot3(keep_fwd, later) + in_fwd
        exponent_bwd = dot3(keep_bwd, earlier) + in_bwd
        for chunk in range(chunks):
            exponent_fwd += jnp.where(chunk_at < chunk, total_fwd[chunk : chunk + 1, :], 0.0)
            exponent_bwd += jnp.where(chunk_at > chunk, total_bwd[chunk : chunk + 1, :], 0.0)
        exponent_fwd = jnp.where(is_before, exponent_fwd, low)
        exponent_bwd = jnp.where(is_after, exponent_bwd, low)
        top_fwd = jnp.max(jnp.max(exponent_fwd, axis=1, keepdims=True), axis=0, keepdims=True)
        top_bwd = jnp.max(jnp.max(exponent_bwd, axis=1, keepdims=True), axis=0, keepdims=True)
        decay_all[...] = jnp.where(
            is_before,
            jnp.exp(exponent_fwd - top_fwd),
            jnp.where(is_after, jnp.exp(exponent_bwd - top_bwd), 0.0),
        )
        run_fwd = jnp.broadcast_to(own_upto[in_row[1] : in_row[1] + 1, :], (rows, rows))
        run_bwd = jnp.broadcast_to(own_before[in_row[3] : in_row[3] + 1, :], (rows, rows))
        fwd_t, bwd_t = run_fwd.T, run_bwd.T
        log_fwd = jnp.where(
            at_row >= at_col, fwd_t - run_fwd + own[in_row[0] : in_row[0] + 1, :], low
        )
        log_bwd = jnp.where(
            at_row <= at_col, run_bwd - bwd_t + own[in_row[2] : in_row[2] + 1, :], low
        )
        own_total = jnp.sum(own[in_row[3] : in_row[3] + 1, :], axis=1, keepdims=True)
        carry_fwd = fwd_t[:, :1] + top_fwd
        carry_bwd = own_total - bwd_t[:, :1] + top_bwd
        most_fwd = jnp.maximum(jnp.max(log_fwd, axis=1, keepdims=True), carry_fwd)
        most_bwd = jnp.maximum(jnp.max(log_bwd, axis=1, keepdims=True), carry_bwd)
        carry_fwd = jnp.exp(carry_fwd - most_fwd)
        carry_bwd = jnp.exp(carry_bwd - most_bwd)

        if head % 2 == 0:
            depth, start = wide, pair * wide
            query = query_wide[:, start : start + depth]
        else:
            depth, start = narrow, pair * narrow
            query = query_narrow[:, start : start + depth]
            start += heads * wide
        scale = float(depth) ** -0.5
        value_at = heads * (wide + narrow) + head * width
        sum_fwd = sum_bwd = None
        own_scores = None
        for index, (source, block) in enumerate(zip(sources, blocks)):
            scores = (
                lax.dot_general(
                    query,
                    block[:rows, start : start + depth],
                    (((1,), (1,)), ((), ())),
                    preferred_element_type=f32,
                )
                * scale
            )
            if index == 0:
                own_scores = scores
                continue
            scores = scores * decay_all[pl.ds(source, 1), :]
            weighted[index] = scores
            ahead = (source < here).astype(f32)
            fwd, bwd = scores * ahead, scores * (1.0 - ahead)
            sum_fwd = fwd if sum_fwd is None else sum_fwd + fwd
            sum_bwd = bwd if sum_bwd is None else sum_bwd + bwd
        own_fwd = own_scores * jnp.exp(log_fwd - most_fwd)
        own_bwd = own_scores * jnp.exp(log_bwd - most_bwd)
        divide_fwd = jnp.sum(carry_fwd * sum_fwd + own_fwd, axis=1, keepdims=True)
        divide_bwd = jnp.sum(carry_bwd * sum_bwd + own_bwd, axis=1, keepdims=True)
        divide_fwd = jnp.maximum(jnp.maximum(jnp.abs(divide_fwd), jnp.exp(-most_fwd)), tiny)
        divide_bwd = jnp.maximum(jnp.maximum(jnp.abs(divide_bwd), jnp.exp(-most_bwd)), tiny)
        carry_fwd = carry_fwd / divide_fwd
        carry_bwd = carry_bwd / divide_bwd
        cell = jnp.zeros((rows, width), f32)
        for index, (source, block) in enumerate(zip(sources, blocks)):
            if index == 0:
                scores = own_fwd / divide_fwd + own_bwd / divide_bwd
            else:
                scores = weighted[index] * jnp.where(source < here, carry_fwd, carry_bwd)
            upper = scores.astype(bf16)
            lower = (scores - upper.astype(f32)).astype(bf16)
            value = block[:rows, value_at : value_at + width]
            cell += jnp.dot(upper, value, preferred_element_type=f32)
            cell += jnp.dot(lower, value, preferred_element_type=f32)
        mean = jnp.mean(cell * cell, axis=1, keepdims=True)
        columns = slice(head * width, (head + 1) * width)
        cell = cell * lax.rsqrt(mean + norm_eps) * gain_all[:, columns]
        merged[:, columns] = (residual[:, columns].astype(f32) + cell).astype(bf16)

    table[...] = route_table(routes, chunks)
    rows_out = merged[...]
    for step, target in enumerate(sent):
        picked = select_rows(table, here ^ step, capacity)
        target[...] = jnp.dot(picked, rows_out, preferred_element_type=f32).astype(bf16)


def expert_kernel(parts, tile, *refs):
    pieces = refs[:parts]
    norm_gain, gate, up, down = refs[parts : parts + 4]
    outs = refs[parts + 4 : 2 * parts + 4]
    normed, hidden = refs[2 * parts + 4 :]
    rows, width = pieces[0].shape
    here = lax.axis_index("tp")
    squares = None
    for piece in pieces:
        part = piece[...].astype(f32)
        part = jnp.sum(part * part, axis=1, keepdims=True)
        squares = part if squares is None else squares + part
    scale = lax.rsqrt(squares / (width * parts) + norm_eps)
    for index, piece in enumerate(pieces):
        at = pl.multiple_of((here ^ index) * width, width)
        part = piece[...].astype(f32) * scale * norm_gain[:, pl.ds(at, width)]
        normed[:, pl.ds(at, width)] = part.astype(bf16)
    units = gate.shape[1]
    for start in range(0, units, tile):
        stop = min(start + tile, units)
        first = jnp.dot(normed[...], gate[:, start:stop], preferred_element_type=f32)
        second = jnp.dot(normed[...], up[:, start:stop], preferred_element_type=f32)
        hidden[:, start:stop] = (first * jax.nn.sigmoid(first) * second).astype(bf16)
    for index, out in enumerate(outs):
        for start in range(0, width, tile):
            at = pl.multiple_of((here ^ index) * width + start, 128)
            stop = min(start + tile, width)
            value = jnp.dot(
                hidden[...], down[:, pl.ds(at, stop - start)], preferred_element_type=f32
            )
            out[:, start:stop] = value.astype(bf16)


def combine_kernel(chunks, *refs):
    merged, routes, picks, weights = refs[:4]
    back = refs[4 : 4 + chunks]
    out, table = refs[4 + chunks :]
    here = lax.axis_index("sp")
    table[...] = route_table(routes, chunks)
    total = merged[...].astype(f32)
    pick_all, weight_all = picks[...], weights[...]
    for step, block in enumerate(back):
        expert = here ^ step
        picked = select_rows(table, expert, block.shape[0])
        rows = lax.dot_general(
            picked, block[...], (((0,), (0,)), ((), ())), preferred_element_type=f32
        )
        weight = jnp.sum(jnp.where(pick_all == expert, weight_all, 0.0), axis=1, keepdims=True)
        total = total + rows * weight
    out[...] = total.astype(bf16)


def body(
    sp_size,
    tp_size,
    residual,
    query_wide,
    key_wide,
    query_narrow,
    key_narrow,
    values,
    gate_logits,
    head_gain,
    norm_gain,
    route_experts,
    route_weights,
    expert_gate,
    expert_up,
    expert_down,
):
    tokens, own_width = residual.shape
    heads = gate_logits.shape[1] // 2
    wide, narrow = query_wide.shape[1] // heads, query_narrow.shape[1] // heads
    width = values.shape[1] // (2 * heads)
    tops = route_experts.shape[1]
    capacity = 2 * tops * tokens // sp_size
    shape = jax.ShapeDtypeStruct

    def over_sp(array, target):
        return lax.ppermute(array, "sp", [(i, target(i)) for i in range(sp_size)])

    def over_tp(array, bit):
        return lax.ppermute(array, "tp", [(i, i ^ bit) for i in range(tp_size)])

    gate_rows = gate_logits.shape[0] * gate_logits.shape[1]
    packed_width = key_wide.shape[1] + key_narrow.shape[1] + values.shape[1]
    packed = call(
        pack_kernel,
        shape((tokens + gate_rows, packed_width), bf16),
        (key_wide, key_narrow, values, gate_logits),
        nbytes=tokens * packed_width * 4,
    )
    lines = sp_size // 2
    blocks = [packed, over_sp(packed, lambda i: i ^ 1)]
    for turn in range(1, lines):
        moved = over_sp(packed, lambda i: (i + 2 * turn) % sp_size)
        blocks += [moved, over_sp(moved, lambda i: i ^ 1)]
    routes = route_experts.T

    outs = [shape((tokens, own_width), bf16)]
    outs += [shape((capacity, own_width), bf16)] * sp_size
    merged, *sent = call(
        functools.partial(cell_kernel, heads, wide, narrow, width, sp_size, capacity),
        outs,
        (query_wide, query_narrow, residual, head_gain[None, :], routes, *blocks),
        scratch=[
            pltpu.VMEM((gate_rows, sp_size, tokens), f32),
            pltpu.VMEM((sp_size, tokens), f32),
            pltpu.VMEM((sp_size, tokens, tokens), f32),
            pltpu.VMEM((sp_size, tokens), f32),
        ],
        flops=2 * tokens * tokens * sp_size * 6 * (wide + narrow + 4 * width),
        nbytes=tokens * packed_width * 2 * sp_size,
    )
    arrived = [sent[0]]
    arrived += [over_sp(sent[step], lambda i: i ^ step) for step in range(1, sp_size)]
    pieces = {0: jnp.concatenate(arrived, axis=0)}
    bit = tp_size // 2
    while bit:
        for index in list(pieces):
            pieces[index | bit] = over_tp(pieces[index], bit)
        bit //= 2
    pieces = [pieces[index] for index in range(tp_size)]
    slots = sp_size * capacity
    units = expert_gate.shape[2]
    model = own_width * tp_size
    partial = call(
        functools.partial(expert_kernel, tp_size, 256),
        [shape((slots, own_width), bf16)] * tp_size,
        (*pieces, norm_gain[None, :], expert_gate[0], expert_up[0], expert_down[0]),
        scratch=[pltpu.VMEM((slots, model), bf16), pltpu.VMEM((slots, units), bf16)],
        flops=6 * slots * model * units,
        nbytes=6 * model * units + 8 * slots * model,
    )
    partial = dict(enumerate(partial))
    bit = 1
    while bit < tp_size:
        for index in [i for i in partial if not i & bit]:
            moved = over_tp(partial.pop(index | bit), bit)
            partial[index] = (partial[index].astype(f32) + moved.astype(f32)).astype(bf16)
        bit *= 2
    summed = partial[0].reshape(sp_size, capacity, own_width)
    back = [summed[0]]
    back += [over_sp(summed[step], lambda i: i ^ step) for step in range(1, sp_size)]
    return call(
        functools.partial(combine_kernel, sp_size),
        shape((tokens, own_width), bf16),
        (merged, routes, route_experts, route_weights, *back),
        scratch=[pltpu.VMEM((sp_size, tokens), f32)],
        flops=2 * tokens * slots * own_width,
        nbytes=slots * own_width * 2,
    )


def solution(mesh):
    return jax.shard_map(
        functools.partial(body, mesh.shape["sp"], mesh.shape["tp"]),
        mesh=mesh,
        in_specs=(
            P("sp", "tp"),
            P("sp", "tp"),
            P("sp", "tp"),
            P("sp", "tp"),
            P("sp", "tp"),
            P("sp", "tp"),
            P(None, "tp", "sp"),
            P("tp"),
            P(),
            P("sp", None),
            P("sp", None),
            P("sp", None, "tp"),
            P("sp", None, "tp"),
            P("sp", "tp", None),
        ),
        out_specs=P("sp", "tp"),
        check_vma=False,
    )
```
